32 devices in a mesh: sp: 4 (over z), fs: 4 (over y, x), tp: 2 (over core).
Axes of the slice: x: 2, y: 2, z: 4, core: 2. Of those that a mesh axis runs over, the one named last changes fastest.
Arguments:
- tokens: bfloat16 [4096, 2048], P('sp'), may hold values from -6 to 6
- norm_gain: float32 [2048], replicated, may hold values from 0.1 to 1.9
- w_query: bfloat16 [2048, 2048], P('sp', ('fs', 'tp')), may hold values from -3.6239223 to 3.6239223
- w_key: bfloat16 [2048, 512], P('sp', ('fs', 'tp')), may hold values from -0.088388348 to 0.088388348
- w_value: bfloat16 [2048, 512], P('sp', ('fs', 'tp')), may hold values from -0.8984375 to 0.8984375
- w_conv_in: bfloat16 [2048, 2048], P('sp', ('fs', 'tp')), may hold values from -0.125 to 0.125
- w_conv_gate: bfloat16 [2048, 2048], P('sp', ('fs', 'tp')), may hold values from -0.125 to 0.125
- conv_taps: bfloat16 [3, 2048], P(None, ('fs', 'tp')), may hold values from -3.5 to 3.5
- sink_logits: float32 [32], P(('fs', 'tp')), may hold values from 2 to 6
Outputs:
- mixed: bfloat16 [4096, 2048], P('sp', ('fs', 'tp'))
- log_sums: float32 [32, 4096], P(('fs', 'tp'), 'sp')
The draws below stay inside these ranges and needn't reach their ends.
All inputs are finite; a program needn't handle non-finite values.
Results may differ from the reference program's by a relative error of at most 0.0077.
Values may be sent and summed in bfloat16 or wider, within the bound.
A program may use at most 64 MiB of HBM per device.

```python
import math
import jax
import jax.numpy as jnp
from jax import lax

HEAD_DIM = 64
KV_HEADS = 8
GROUP = 4
HEADS = 32
D = 2048
WINDOW = 128
TAPS = 3
TOKENS = 4096


def shared_key_weight(key):
    base_draw = jax.random.normal(jax.random.fold_in(key, 101), (D, KV_HEADS * HEAD_DIM), jnp.float32)
    return jnp.clip(base_draw, -4.0, 4.0) / math.sqrt(D)


def draw_w_key(key, part):
    return shared_key_weight(key).astype(jnp.bfloat16)


def draw_w_query(key, part):
    noise_part = jnp.clip(jax.random.normal(jax.random.fold_in(key, 202), (D, HEADS * HEAD_DIM), jnp.float32), -4.0, 4.0) / math.sqrt(D)
    return noise_part.astype(jnp.bfloat16)


def block_levels(rng, extent, pieces, smallest, largest):
    level, own = 1.0, jax.random.fold_in(rng, 6)
    for position, parts in pieces:
        steps = jnp.exp(jax.random.uniform(jax.random.fold_in(own, position), (parts,), jnp.float32, smallest / len(pieces), largest / len(pieces)))
        level = level * jnp.repeat(steps, extent[position] // parts).reshape([-1 if axis == position else 1 for axis in range(len(extent))])
    return level


def noise(stream_key, extent, width, limit, cuts=(), held_as=jnp.bfloat16):
    result = width * jax.random.normal(stream_key, extent, jnp.float32)
    if cuts:
        result = result * block_levels(stream_key, extent, cuts, -0.22, 0.18)
    return jnp.clip(result, -limit, limit).astype(held_as)


def setup_inputs(seed: int = 0) -> dict:
    keys = jax.random.split(jax.random.key(seed), 10)
    return {
        "tokens": noise(keys[0], (TOKENS, D), 1.0, 6.0, ((0, 4),)),
        "norm_gain": jnp.clip(1.0 + 0.18 * jax.random.normal(keys[1], (D,), jnp.float32), 0.1, 1.9),
        "w_query": draw_w_query(jax.random.fold_in(keys[9], 71), 0),
        "w_key": draw_w_key(jax.random.fold_in(keys[9], 71), 0),
        "w_value": noise(keys[4], (D, KV_HEADS * HEAD_DIM), 0.15, 0.8984375, ((0, 4), (1, 8))),
        "w_conv_in": noise(keys[5], (D, D), D ** -0.5, 0.125, ((0, 4), (1, 8))),
        "w_conv_gate": noise(keys[6], (D, D), D ** -0.5, 0.125, ((0, 4), (1, 8))),
        "conv_taps": noise(keys[7], (TAPS, D), TAPS ** -0.5, 3.5, ((1, 8),)),
        "sink_logits": jnp.clip(2.0 + 4.0 * jax.random.uniform(keys[8], (HEADS,), jnp.float32) ** block_levels(keys[8], (HEADS,), ((0, 8),), -0.2, 0.2), 2.0, 6.0),
    }


EPS = 1e-06

def attend_group(query_blocks, key_span, value_span, sink_group, in_window):
    scores = jnp.einsum('nqgd,nkd->ngqk', query_blocks.astype(jnp.float32), key_span.astype(jnp.float32)) * HEAD_DIM ** (-0.5)
    scores = jnp.where(in_window[:, None], scores, -jnp.inf)
    sink_col = sink_group[None, :, None, None]
    row_top = jnp.maximum(lax.optimization_barrier(jnp.max(scores, axis=-1, keepdims=True)), sink_col)
    raised = jnp.exp(scores - row_top)
    row_sum = lax.optimization_barrier(jnp.sum(raised, axis=-1, keepdims=True)) + jnp.exp(sink_col - row_top)
    soft_weights = (raised / row_sum).astype(jnp.bfloat16)
    attended = jnp.einsum('ngqk,nkd->nqgd', soft_weights.astype(jnp.float32), value_span.astype(jnp.float32))
    return (attended, (row_top + jnp.log(row_sum))[..., 0])

def block_spans(rows_bf, blocks):
    shaped = rows_bf.reshape(blocks, WINDOW, KV_HEADS, HEAD_DIM)
    earlier = jnp.concatenate([jnp.zeros_like(shaped[:1]), shaped[:-1]], axis=0)
    return jnp.concatenate([earlier, shaped], axis=1).transpose(2, 0, 1, 3)

def reference(tokens, norm_gain, w_query, w_key, w_value, w_conv_in, w_conv_gate, conv_taps, sink_logits):
    widened = tokens.astype(jnp.float32)
    normed = (widened * lax.rsqrt(lax.optimization_barrier(jnp.mean(widened * widened, axis=-1, keepdims=True)) + EPS) * norm_gain).astype(jnp.bfloat16)
    query, key_rows, value_rows, conv_in, conv_gate = [jnp.dot(normed, weight, preferred_element_type=jnp.float32).astype(jnp.bfloat16) for weight in (w_query, w_key, w_value, w_conv_in, w_conv_gate)]
    blocks = TOKENS // WINDOW
    query_blocks = query.reshape(blocks, WINDOW, KV_HEADS, GROUP, HEAD_DIM).transpose(2, 0, 1, 3, 4)
    query_idx = jnp.arange(WINDOW)[:, None] + WINDOW
    key_idx = jnp.arange(2 * WINDOW)[None, :]
    offset_gap = query_idx - key_idx
    in_band = (offset_gap >= 0) & (offset_gap < WINDOW)
    block_idx = jnp.arange(blocks)[:, None, None]
    in_window = in_band[None] & ((block_idx > 0) | (key_idx[None] >= WINDOW))
    sink_table = sink_logits.reshape(KV_HEADS, GROUP)
    attended, log_sums = lax.map(lambda group_args: attend_group(group_args[0], group_args[1], group_args[2], group_args[3], in_window), (query_blocks, block_spans(key_rows, blocks), block_spans(value_rows, blocks), sink_table))
    attended = attended.transpose(1, 2, 0, 3, 4).reshape(TOKENS, HEADS * HEAD_DIM)
    log_sums = log_sums.transpose(0, 2, 1, 3).reshape(HEADS, TOKENS)
    padded = jnp.concatenate([jnp.zeros((TAPS - 1, D), jnp.bfloat16), conv_in], axis=0)
    conv_sum = jnp.zeros((TOKENS, D), jnp.float32)
    for tap_idx in range(TAPS):
        conv_sum = conv_sum + conv_taps[tap_idx].astype(jnp.float32) * padded[tap_idx:tap_idx + TOKENS].astype(jnp.float32)
    convolved = conv_gate.astype(jnp.float32) * conv_sum
    mixed = (attended + convolved).astype(jnp.bfloat16)
    return (mixed, log_sums)
```

```python
import functools

import jax
import jax.numpy as jnp
from jax import lax
from jax.experimental import pallas as pl
from jax.experimental.pallas import tpu as pltpu
from jax.sharding import PartitionSpec as P

HEAD_DIM = 64
WINDOW = 128
TAPS = 3
EPS = 1e-06
LANES = 128
PAD = 8
MESH = pl.DeviceIdType.MESH


def kernel(
    n,
    tok_ref, gain_ref, wkv_ref, wq_ref, wci_ref, wcg_ref, taps_ref, sink_ref,
    mixed_ref, log_ref,
    tok, normed, kv_all, q_all, ci_all, cg_all, kv, query, attended, conv_in,
    tok_sem, own_sem, recv_sem, right_sem, left_sem, halo_send, halo_recv,
):
    me = lax.axis_index("sp")
    rows = tok.shape[0]
    depth = wq_ref.shape[0]
    shards = (wkv_ref, wq_ref, wci_ref, wcg_ref)
    wholes = (kv_all, q_all, ci_all, cg_all)
    has_left, has_right = me > 0, me < n - 1
    left, right = jnp.maximum(me - 1, 0), jnp.minimum(me + 1, n - 1)
    blocks = rows // WINDOW
    f32, bf16 = jnp.float32, jnp.bfloat16

    step_rows = rows // 4
    tok_copies = [
        pltpu.make_async_copy(
            tok_ref.at[pl.ds(i * step_rows, step_rows)], tok.at[pl.ds(i * step_rows, step_rows)], tok_sem.at[i]
        )
        for i in range(4)
    ]
    for copy in tok_copies:
        copy.start()

    def place(a, shard):
        return wholes[a].at[pl.ds(pl.multiple_of(shard * depth, depth), depth)]

    own_copies = [pltpu.make_async_copy(shards[a], place(a, me), own_sem.at[a]) for a in range(4)]
    for copy in own_copies:
        copy.start()

    barrier = pltpu.get_barrier_semaphore()

    @pl.when(has_left)
    def _():
        pl.semaphore_signal(barrier, inc=1, device_id={"sp": left}, device_id_type=MESH)

    @pl.when(has_right)
    def _():
        pl.semaphore_signal(barrier, inc=1, device_id={"sp": right}, device_id_type=MESH)

    pl.semaphore_wait(barrier, has_left.astype(jnp.int32) + has_right.astype(jnp.int32))

    def hop(a, shard, to_right, own=False):
        return pltpu.make_async_remote_copy(
            src_ref=shards[a] if own else place(a, shard),
            dst_ref=place(a, shard),
            send_sem=(right_sem if to_right else left_sem).at[a, shard],
            recv_sem=recv_sem.at[a, shard],
            device_id={"sp": right if to_right else left},
            device_id_type=MESH,
        )

    def send_own(a):
        @pl.when(has_right)
        def _():
            hop(a, me, True, True).start()

        @pl.when(has_left)
        def _():
            hop(a, me, False, True).start()

    def pass_on(a, first, last):
        def step(k, carry):
            @pl.when(me - k >= 0)
            def _():
                shard = me - k
                hop(a, shard, False).wait_recv()

                @pl.when(has_right)
                def _():
                    hop(a, shard, True).start()

            @pl.when(me + k < n)
            def _():
                shard = me + k
                hop(a, shard, True).wait_recv()

                @pl.when(has_left)
                def _():
                    hop(a, shard, False).start()

            return carry

        lax.fori_loop(first, last, step, 0)

    for a in range(3):
        send_own(a)

    norm_rows = 64
    for i in range(4):
        tok_copies[i].wait()

        @pl.loop(0, step_rows // norm_rows)
        def _(j):
            at = pl.ds(pl.multiple_of(i * step_rows + j * norm_rows, norm_rows), norm_rows)
            wide = tok[at, :].astype(f32)
            scale = lax.rsqrt(jnp.mean(wide * wide, axis=-1, keepdims=True) + EPS)
            normed[at, :] = (wide * scale * gain_ref[...]).astype(bf16)

    for copy in own_copies:
        copy.wait()

    tile = 256

    def project(a, store):
        @pl.loop(0, rows // tile)
        def _(i):
            base = pl.multiple_of(i * tile, tile)
            store(base, jnp.dot(normed[pl.ds(base, tile), :], wholes[a][...], preferred_element_type=f32))

    def halo(buffer, length, i):
        return pltpu.make_async_remote_copy(
            src_ref=buffer.at[pl.ds(rows, length)],
            dst_ref=buffer.at[pl.ds(0, length)],
            send_sem=halo_send.at[i],
            recv_sem=halo_recv.at[i],
            device_id={"sp": right},
            device_id_type=MESH,
        )

    pass_on(0, 1, n)
    send_own(3)

    def store_kv(base, value):
        kv[pl.ds(base + WINDOW, tile), :] = value.astype(bf16)

    project(0, store_kv)

    @pl.when(jnp.logical_not(has_left))
    def _():
        kv[pl.ds(0, WINDOW), :] = jnp.zeros((WINDOW, kv.shape[1]), bf16)
        conv_in[pl.ds(0, PAD), :] = jnp.zeros((PAD, conv_in.shape[1]), f32)

    pass_on(1, 1, n)

    @pl.when(has_right)
    def _():
        halo(kv, WINDOW, 0).start()

    def store_query(base, value):
        query[pl.ds(base, tile), :] = value.astype(bf16)

    project(1, store_query)

    heads = query.shape[1] // HEAD_DIM
    query_idx = lax.broadcasted_iota(jnp.int32, (WINDOW, 2 * WINDOW), 0)
    key_idx = lax.broadcasted_iota(jnp.int32, (WINDOW, 2 * WINDOW), 1)
    gap = query_idx + WINDOW - key_idx
    band = (gap >= 0) & (gap < WINDOW)
    lane = lax.broadcasted_iota(jnp.int32, (2 * WINDOW, LANES), 1)
    low = lane < HEAD_DIM
    stat_lane = lax.broadcasted_iota(jnp.int32, (WINDOW, LANES), 1)

    def attend(b, kept):
        base = pl.multiple_of(b * WINDOW, WINDOW)
        both = kv[pl.ds(base, 2 * WINDOW), :].astype(f32)
        turned = pltpu.roll(both, HEAD_DIM, 1)
        zero = jnp.zeros_like(both)
        keys = (jnp.where(low, both, zero).astype(bf16), jnp.where(low, zero, turned).astype(bf16))
        vals = (jnp.where(low, turned, zero).astype(bf16), jnp.where(low, zero, both).astype(bf16))
        stats = jnp.zeros((WINDOW, LANES), f32)
        for pair in range(heads // 2):
            cols = pl.ds(pair * LANES, LANES)
            q = query[pl.ds(base, WINDOW), cols]
            out = None
            for side in range(2):
                head = 2 * pair + side
                scores = lax.dot_general(
                    q, keys[side], (((1,), (1,)), ((), ())), preferred_element_type=f32
                ) * HEAD_DIM ** (-0.5)
                scores = jnp.where(kept, scores, -jnp.inf)
                sink = jnp.full((WINDOW, 1), sink_ref[head], f32)
                top = jnp.maximum(jnp.max(scores, axis=-1, keepdims=True), sink)
                raised = jnp.exp(scores - top)
                total = jnp.sum(raised, axis=-1, keepdims=True) + jnp.exp(sink - top)
                weights = (raised * (1.0 / total)).astype(bf16)
                part = jnp.dot(weights, vals[side], preferred_element_type=f32)
                out = part if out is None else out + part
                stats = jnp.where(stat_lane == head, top + jnp.log(total), stats)
            attended[pl.ds(base, WINDOW), cols] = out
        log_ref[:, pl.ds(base, WINDOW)] = jnp.transpose(stats)[:heads]

    def attend_range(first, last):
        @pl.loop(first, last)
        def _(b):
            attend(b, band)

    cut = [1 + (n - 1) * i // 3 for i in range(4)]
    mid = 1 + (blocks - 1) // 2
    attend_range(1, mid)
    pass_on(2, cut[0], cut[1])
    attend_range(mid, blocks)
    pass_on(2, cut[1], cut[2])

    @pl.when(has_left)
    def _():
        halo(kv, WINDOW, 0).wait_recv()

    attend(0, band & ((key_idx >= WINDOW) | has_left))
    pass_on(2, cut[2], cut[3])

    def store_conv(base, value):
        conv_in[pl.ds(base + PAD, tile), :] = value.astype(bf16).astype(f32)

    project(2, store_conv)
    pass_on(3, 1, 2)

    @pl.when(has_right)
    def _():
        halo(conv_in, PAD, 1).start()

    pass_on(3, 2, n)

    @pl.when(has_left)
    def _():
        halo(conv_in, PAD, 1).wait_recv()

    def store_mixed(base, value):
        gate = value.astype(bf16).astype(f32)
        taps = taps_ref[...].astype(f32)
        near = conv_in[pl.ds(base, tile + PAD), :]
        total = jnp.zeros_like(gate)
        for k in range(TAPS):
            start = PAD - TAPS + 1 + k
            total = total + taps[k : k + 1] * near[start : start + tile]
        mixed_ref[pl.ds(base, tile), :] = (attended[pl.ds(base, tile), :] + gate * total).astype(bf16)

    project(3, store_mixed)

    @pl.when(has_right)
    def _():
        halo(kv, WINDOW, 0).wait_send()
        halo(conv_in, PAD, 1).wait_send()

    for a in range(4):

        @pl.when(has_right)
        def _():
            @pl.loop(0, me + 1)
            def _(s):
                hop(a, s, True).wait_send()

        @pl.when(has_left)
        def _():
            @pl.loop(me, n)
            def _(s):
                hop(a, s, False).wait_send()


def body(n, tokens, norm_gain, w_query, w_key, w_value, w_conv_in, w_conv_gate, conv_taps, sink_logits):
    rows, features = tokens.shape
    width, kv_width = w_query.shape[1], w_key.shape[1] + w_value.shape[1]
    assert w_key.shape[1] == HEAD_DIM and width % LANES == 0
    w_kv = jnp.concatenate([w_key, w_value], axis=1)
    f32, bf16 = jnp.float32, jnp.bfloat16
    hbm = pl.BlockSpec(memory_space=pltpu.HBM)
    vmem = pl.BlockSpec(memory_space=pltpu.VMEM)
    smem = pl.BlockSpec(memory_space=pltpu.SMEM)
    dma = pltpu.SemaphoreType.DMA
    return pl.pallas_call(
        functools.partial(kernel, n),
        out_shape=(
            jax.ShapeDtypeStruct((rows, width), bf16),
            jax.ShapeDtypeStruct((width // HEAD_DIM, rows), f32),
        ),
        in_specs=[hbm, vmem, hbm, hbm, hbm, hbm, vmem, smem],
        out_specs=(vmem, vmem),
        scratch_shapes=[
            pltpu.VMEM((rows, features), bf16),
            pltpu.VMEM((rows, features), bf16),
            pltpu.VMEM((features, kv_width), bf16),
            pltpu.VMEM((features, width), bf16),
            pltpu.VMEM((features, width), bf16),
            pltpu.VMEM((features, width), bf16),
            pltpu.VMEM((rows + WINDOW, kv_width), bf16),
            pltpu.VMEM((rows, width), bf16),
            pltpu.VMEM((rows, width), f32),
            pltpu.VMEM((rows + PAD, width), f32),
            dma((4,)),
            dma((4,)),
            dma((4, n)),
            dma((4, n)),
            dma((4, n)),
            dma((2,)),
            dma((2,)),
        ],
        compiler_params=pltpu.CompilerParams(
            collective_id=0, has_side_effects=True, vmem_limit_bytes=60 << 20
        ),
        name="gather_attend_convolve",
    )(tokens, norm_gain.reshape(1, -1), w_kv, w_query, w_conv_in, w_conv_gate, conv_taps, sink_logits)


def solution(mesh):
    return jax.shard_map(
        functools.partial(body, mesh.shape["sp"]),
        mesh=mesh,
        in_specs=(
            P("sp", None),
            P(),
            P("sp", ("fs", "tp")),
            P("sp", ("fs", "tp")),
            P("sp", ("fs", "tp")),
            P("sp", ("fs", "tp")),
            P("sp", ("fs", "tp")),
            P(None, ("fs", "tp")),
            P(("fs", "tp")),
        ),
        out_specs=(P("sp", ("fs", "tp")), P(("fs", "tp"), "sp")),
        check_vma=False,
    )
```

```python
import functools

import jax
import jax.numpy as jnp
from jax import lax
from jax.experimental import pallas as pl
from jax.experimental.pallas import tpu as pltpu
from jax.sharding import PartitionSpec as P

HEAD_DIM = 64
WINDOW = 128
TAPS = 3
EPS = 1e-06
LANES = 128
PAD = 8
MESH = pl.DeviceIdType.MESH


def kernel(
    n, flip, tok_ref, gain_ref, *refs
):
    arrays = 5 if flip else 4
    shards = refs[:arrays]
    (
        taps_ref, sink_ref, mixed_ref, log_ref,
        tok, normed, kv_all, q_all, ci_all, cg_all, kv, query, attended, conv_in, gate_sum,
        tok_sem, own_sem, recv_sem, right_sem, left_sem, halo_send, halo_recv,
    ) = refs[arrays:]
    QUERY, CONV, GATE = arrays - 3, arrays - 2, arrays - 1
    me = lax.axis_index("sp")
    rows = tok.shape[0]
    depth = shards[QUERY].shape[0]
    wholes = (kv_all, kv_all, q_all, ci_all, cg_all)[5 - arrays :]
    has_left, has_right = me > 0, me < n - 1
    left, right = jnp.maximum(me - 1, 0), jnp.minimum(me + 1, n - 1)
    blocks = rows // WINDOW
    f32, bf16 = jnp.float32, jnp.bfloat16

    step_rows = rows // 4
    tok_copies = [
        pltpu.make_async_copy(
            tok_ref.at[pl.ds(i * step_rows, step_rows)], tok.at[pl.ds(i * step_rows, step_rows)], tok_sem.at[i]
        )
        for i in range(4)
    ]
    for copy in tok_copies:
        copy.start()

    def place(a, shard):
        at = pl.ds(pl.multiple_of(shard * depth, depth), depth)
        if flip and a < QUERY:
            return kv_all.at[pl.ds(a * HEAD_DIM, HEAD_DIM), at]
        return wholes[a].at[at]

    own_copies = [pltpu.make_async_copy(shards[a], place(a, me), own_sem.at[a]) for a in range(arrays)]
    for copy in own_copies:
        copy.start()

    barrier = pltpu.get_barrier_semaphore()

    @pl.when(has_left)
    def _():
        pl.semaphore_signal(barrier, inc=1, device_id={"sp": left}, device_id_type=MESH)

    @pl.when(has_right)
    def _():
        pl.semaphore_signal(barrier, inc=1, device_id={"sp": right}, device_id_type=MESH)

    pl.semaphore_wait(barrier, has_left.astype(jnp.int32) + has_right.astype(jnp.int32))

    def hop(a, shard, to_right, own=False):
        return pltpu.make_async_remote_copy(
            src_ref=shards[a] if own else place(a, shard),
            dst_ref=place(a, shard),
            send_sem=(right_sem if to_right else left_sem).at[a, shard],
            recv_sem=recv_sem.at[a, shard],
            device_id={"sp": right if to_right else left},
            device_id_type=MESH,
        )

    def send_own(a):
        @pl.when(has_right)
        def _():
            hop(a, me, True, True).start()

        @pl.when(has_left)
        def _():
            hop(a, me, False, True).start()

    def pass_on(a, first, last):
        def step(k, carry):
            @pl.when(me - k >= 0)
            def _():
                shard = me - k
                hop(a, shard, False).wait_recv()

                @pl.when(has_right)
                def _():
                    hop(a, shard, True).start()

            @pl.when(me + k < n)
            def _():
                shard = me + k
                hop(a, shard, True).wait_recv()

                @pl.when(has_left)
                def _():
                    hop(a, shard, False).start()

            return carry

        lax.fori_loop(first, last, step, 0)

    for a in range(GATE):
        send_own(a)

    norm_rows = 64
    for i in range(4):
        tok_copies[i].wait()

        @pl.loop(0, step_rows // norm_rows)
        def _(j):
            at = pl.ds(pl.multiple_of(i * step_rows + j * norm_rows, norm_rows), norm_rows)
            wide = tok[at, :].astype(f32)
            scale = lax.rsqrt(jnp.mean(wide * wide, axis=-1, keepdims=True) + EPS)
            normed[at, :] = (wide * scale * gain_ref[...]).astype(bf16)

    for copy in own_copies:
        copy.wait()

    tile = 256

    def project(a, store):
        @pl.loop(0, rows // tile)
        def _(i):
            base = pl.multiple_of(i * tile, tile)
            side = 1 if flip and a < QUERY else 0
            store(
                base,
                lax.dot_general(
                    normed[pl.ds(base, tile), :],
                    wholes[a][...],
                    (((1,), (side,)), ((), ())),
                    preferred_element_type=f32,
                ),
            )

    def halo(buffer, length, i):
        return pltpu.make_async_remote_copy(
            src_ref=buffer.at[pl.ds(rows, length)],
            dst_ref=buffer.at[pl.ds(0, length)],
            send_sem=halo_send.at[i],
            recv_sem=halo_recv.at[i],
            device_id={"sp": right},
            device_id_type=MESH,
        )

    for a in range(QUERY):
        pass_on(a, 1, n)
    send_own(GATE)

    def store_kv(base, value):
        kv[pl.ds(base + WINDOW, tile), :] = value.astype(bf16)

    project(0, store_kv)

    @pl.when(jnp.logical_not(has_left))
    def _():
        kv[pl.ds(0, WINDOW), :] = jnp.zeros((WINDOW, kv.shape[1]), bf16)
        conv_in[pl.ds(0, PAD), :] = jnp.zeros((PAD, conv_in.shape[1]), f32)

    pass_on(QUERY, 1, n)

    @pl.when(has_right)
    def _():
        halo(kv, WINDOW, 0).start()

    def store_query(base, value):
        query[pl.ds(base, tile), :] = value.astype(bf16)

    project(QUERY, store_query)

    heads = query.shape[1] // HEAD_DIM
    query_idx = lax.broadcasted_iota(jnp.int32, (WINDOW, 2 * WINDOW), 0)
    key_idx = lax.broadcasted_iota(jnp.int32, (WINDOW, 2 * WINDOW), 1)
    gap = query_idx + WINDOW - key_idx
    band = (gap >= 0) & (gap < WINDOW)
    lane = lax.broadcasted_iota(jnp.int32, (2 * WINDOW, LANES), 1)
    low = lane < HEAD_DIM
    stat_lane = lax.broadcasted_iota(jnp.int32, (WINDOW, LANES), 1)

    def attend(b, kept):
        base = pl.multiple_of(b * WINDOW, WINDOW)
        both = kv[pl.ds(base, 2 * WINDOW), :].astype(f32)
        turned = pltpu.roll(both, HEAD_DIM, 1)
        zero = jnp.zeros_like(both)
        keys = (jnp.where(low, both, zero).astype(bf16), jnp.where(low, zero, turned).astype(bf16))
        vals = (jnp.where(low, turned, zero).astype(bf16), jnp.where(low, zero, both).astype(bf16))
        stats = jnp.zeros((WINDOW, LANES), f32)
        for pair in range(heads // 2):
            cols = pl.ds(pair * LANES, LANES)
            q = query[pl.ds(base, WINDOW), cols]
            out = None
            for side in range(2):
                head = 2 * pair + side
                scores = lax.dot_general(
                    q, keys[side], (((1,), (1,)), ((), ())), preferred_element_type=f32
                ) * HEAD_DIM ** (-0.5)
                scores = jnp.where(kept, scores, -jnp.inf)
                sink = jnp.full((WINDOW, 1), sink_ref[head], f32)
                top = jnp.maximum(jnp.max(scores, axis=-1, keepdims=True), sink)
                raised = jnp.exp(scores - top)
                total = jnp.sum(raised, axis=-1, keepdims=True) + jnp.exp(sink - top)
                weights = (raised * (1.0 / total)).astype(bf16)
                part = jnp.dot(weights, vals[side], preferred_element_type=f32)
                out = part if out is None else out + part
                stats = jnp.where(stat_lane == head, top + jnp.log(total), stats)
            attended[pl.ds(base, WINDOW), cols] = out
        log_ref[:, pl.ds(base, WINDOW)] = jnp.transpose(stats)[:heads]

    def attend_range(first, last):
        @pl.loop(first, last)
        def _(b):
            attend(b, band)

    cut = [1 + (n - 1) * i // 3 for i in range(4)]
    mid = 1 + (blocks - 1) // 2
    attend_range(1, mid)
    pass_on(CONV, cut[0], cut[1])
    attend_range(mid, blocks)
    pass_on(CONV, cut[1], cut[2])

    @pl.when(has_left)
    def _():
        halo(kv, WINDOW, 0).wait_recv()

    attend(0, band & ((key_idx >= WINDOW) | has_left))
    pass_on(CONV, cut[2], cut[3])

    def store_conv(base, value):
        conv_in[pl.ds(base + PAD, tile), :] = value.astype(bf16).astype(f32)

    project(CONV, store_conv)
    early = min(2, n - 1)
    pass_on(GATE, 1, early)

    @pl.when(has_right)
    def _():
        halo(conv_in, PAD, 1).start()

    pass_on(GATE, early, n - 1)

    far = jnp.where(2 * me >= n, 0, n - 1)

    def gate_part(base, shard):
        at = pl.ds(pl.multiple_of(shard * depth, depth), depth)
        return jnp.dot(
            normed[pl.ds(base, tile), at], cg_all[at, :], preferred_element_type=f32
        )

    if flip:

        @pl.loop(0, rows // tile)
        def _(i):
            base = pl.multiple_of(i * tile, tile)
            part = gate_part(base, lax.rem(far + 1, n))
            for j in range(2, n):
                part = part + gate_part(base, lax.rem(far + j, n))
            gate_sum[pl.ds(base, tile), :] = part

    pass_on(GATE, n - 1, n)

    @pl.when(has_left)
    def _():
        halo(conv_in, PAD, 1).wait_recv()

    def store_mixed(base, value):
        gate = value.astype(bf16).astype(f32)
        taps = taps_ref[...].astype(f32)
        near = conv_in[pl.ds(base, tile + PAD), :]
        total = jnp.zeros_like(gate)
        for k in range(TAPS):
            start = PAD - TAPS + 1 + k
            total = total + taps[k : k + 1] * near[start : start + tile]
        mixed_ref[pl.ds(base, tile), :] = (attended[pl.ds(base, tile), :] + gate * total).astype(bf16)

    if flip:

        @pl.loop(0, rows // tile)
        def _(i):
            base = pl.multiple_of(i * tile, tile)
            store_mixed(base, gate_sum[pl.ds(base, tile), :] + gate_part(base, far))

    else:
        project(GATE, store_mixed)

    @pl.when(has_right)
    def _():
        halo(kv, WINDOW, 0).wait_send()
        halo(conv_in, PAD, 1).wait_send()

    for a in range(arrays):

        @pl.when(has_right)
        def _():
            @pl.loop(0, me + 1)
            def _(s):
                hop(a, s, True).wait_send()

        @pl.when(has_left)
        def _():
            @pl.loop(me, n)
            def _(s):
                hop(a, s, False).wait_send()


def body(n, tokens, norm_gain, w_query, w_key, w_value, w_conv_in, w_conv_gate, conv_taps, sink_logits):
    rows, features = tokens.shape
    width, kv_width = w_query.shape[1], w_key.shape[1] + w_value.shape[1]
    assert w_key.shape[1] == HEAD_DIM and width % LANES == 0
    depth = w_query.shape[0]
    flip = depth % LANES == 0 and 2 < n <= 16
    if flip:
        w_kv, kv_shape = (w_key.T, w_value.T), (kv_width, features)
    else:
        w_kv, kv_shape = (jnp.concatenate([w_key, w_value], axis=1),), (features, kv_width)
    arrays = 3 + len(w_kv)
    f32, bf16 = jnp.float32, jnp.bfloat16
    hbm = pl.BlockSpec(memory_space=pltpu.HBM)
    vmem = pl.BlockSpec(memory_space=pltpu.VMEM)
    smem = pl.BlockSpec(memory_space=pltpu.SMEM)
    dma = pltpu.SemaphoreType.DMA
    return pl.pallas_call(
        functools.partial(kernel, n, flip),
        out_shape=(
            pltpu.VMEM((rows, width), bf16),
            pltpu.VMEM((width // HEAD_DIM, rows), f32),
        ),
        in_specs=[hbm, vmem] + [hbm] * arrays + [vmem, smem],
        out_specs=(vmem, vmem),
        scratch_shapes=[
            pltpu.VMEM((rows, features), bf16),
            pltpu.VMEM((rows, features), bf16),
            pltpu.VMEM(kv_shape, bf16),
            pltpu.VMEM((features, width), bf16),
            pltpu.VMEM((features, width), bf16),
            pltpu.VMEM((features, width), bf16),
            pltpu.VMEM((rows + WINDOW, kv_width), bf16),
            pltpu.VMEM((rows, width), bf16),
            pltpu.VMEM((rows, width), f32),
            pltpu.VMEM((rows + PAD, width), f32),
            pltpu.VMEM((rows, width), f32),
            dma((4,)),
            dma((arrays,)),
            dma((arrays, n)),
            dma((arrays, n)),
            dma((arrays, n)),
            dma((2,)),
            dma((2,)),
        ],
        compiler_params=pltpu.CompilerParams(
            collective_id=0, has_side_effects=True, vmem_limit_bytes=59 << 20
        ),
        name="gather_attend_convolve",
    )(tokens, norm_gain.reshape(1, -1), *w_kv, w_query, w_conv_in, w_conv_gate, conv_taps, sink_logits)


def solution(mesh):
    return jax.shard_map(
        functools.partial(body, mesh.shape["sp"]),
        mesh=mesh,
        in_specs=(
            P("sp", None),
            P(),
            P("sp", ("fs", "tp")),
            P("sp", ("fs", "tp")),
            P("sp", ("fs", "tp")),
            P("sp", ("fs", "tp")),
            P("sp", ("fs", "tp")),
            P(None, ("fs", "tp")),
            P(("fs", "tp")),
        ),
        out_specs=(P("sp", ("fs", "tp")), P(("fs", "tp"), "sp")),
        check_vma=False,
    )
```

```python
import functools

import jax
import jax.numpy as jnp
from jax import lax
from jax.experimental import pallas as pl
from jax.experimental.pallas import tpu as pltpu
from jax.sharding import PartitionSpec as P

HEAD_DIM = 64
WINDOW = 128
TAPS = 3
EPS = 1e-06
LANES = 128
PAD = 8
MESH = pl.DeviceIdType.MESH


def kernel(
    n, flip, tok_ref, gain_ref, *refs
):
    arrays = 5 if flip else 4
    shards = refs[:arrays]
    (
        taps_ref, sink_ref, mixed_ref, log_ref,
        tok, normed, kv_all, q_all, ci_all, cg_all, kv, query, attended, conv_in, gate_sum,
        tok_sem, own_sem, recv_sem, right_sem, left_sem, halo_send, halo_recv,
    ) = refs[arrays:]
    QUERY, CONV, GATE = arrays - 3, arrays - 2, arrays - 1
    me = lax.axis_index("sp")
    rows = tok.shape[0]
    depth = shards[QUERY].shape[0]
    wholes = (kv_all, kv_all, q_all, ci_all, cg_all)[5 - arrays :]
    has_left, has_right = me > 0, me < n - 1
    left, right = jnp.maximum(me - 1, 0), jnp.minimum(me + 1, n - 1)
    blocks = rows // WINDOW
    f32, bf16 = jnp.float32, jnp.bfloat16

    step_rows = rows // 4
    tok_copies = [
        pltpu.make_async_copy(
            tok_ref.at[pl.ds(i * step_rows, step_rows)], tok.at[pl.ds(i * step_rows, step_rows)], tok_sem.at[i]
        )
        for i in range(4)
    ]
    for copy in tok_copies:
        copy.start()

    def place(a, shard):
        at = pl.ds(pl.multiple_of(shard * depth, depth), depth)
        if flip and a < QUERY:
            return kv_all.at[pl.ds(a * HEAD_DIM, HEAD_DIM), at]
        return wholes[a].at[at]

    own_copies = [pltpu.make_async_copy(shards[a], place(a, me), own_sem.at[a]) for a in range(arrays)]
    for copy in own_copies:
        copy.start()

    barrier = pltpu.get_barrier_semaphore()

    @pl.when(has_left)
    def _():
        pl.semaphore_signal(barrier, inc=1, device_id={"sp": left}, device_id_type=MESH)

    @pl.when(has_right)
    def _():
        pl.semaphore_signal(barrier, inc=1, device_id={"sp": right}, device_id_type=MESH)

    pl.semaphore_wait(barrier, has_left.astype(jnp.int32) + has_right.astype(jnp.int32))

    def hop(a, shard, to_right, own=False):
        return pltpu.make_async_remote_copy(
            src_ref=shards[a] if own else place(a, shard),
            dst_ref=place(a, shard),
            send_sem=(right_sem if to_right else left_sem).at[a, shard],
            recv_sem=recv_sem.at[a, shard],
            device_id={"sp": right if to_right else left},
            device_id_type=MESH,
        )

    def send_own(a):
        @pl.when(has_right)
        def _():
            hop(a, me, True, True).start()

        @pl.when(has_left)
        def _():
            hop(a, me, False, True).start()

    def pass_on(a, first, last):
        def step(k, carry):
            @pl.when(me - k >= 0)
            def _():
                shard = me - k
                hop(a, shard, False).wait_recv()

                @pl.when(has_right)
                def _():
                    hop(a, shard, True).start()

            @pl.when(me + k < n)
            def _():
                shard = me + k
                hop(a, shard, True).wait_recv()

                @pl.when(has_left)
                def _():
                    hop(a, shard, False).start()

            return carry

        lax.fori_loop(first, last, step, 0)

    for a in range(arrays):
        send_own(a)

    norm_rows = 64
    for i in range(4):
        tok_copies[i].wait()

        @pl.loop(0, step_rows // norm_rows)
        def _(j):
            at = pl.ds(pl.multiple_of(i * step_rows + j * norm_rows, norm_rows), norm_rows)
            wide = tok[at, :].astype(f32)
            scale = lax.rsqrt(jnp.mean(wide * wide, axis=-1, keepdims=True) + EPS)
            normed[at, :] = (wide * scale * gain_ref[...]).astype(bf16)

    for copy in own_copies:
        copy.wait()

    tile = 256

    def project(a, store):
        @pl.loop(0, rows // tile)
        def _(i):
            base = pl.multiple_of(i * tile, tile)
            side = 1 if flip and a < QUERY else 0
            store(
                base,
                lax.dot_general(
                    normed[pl.ds(base, tile), :],
                    wholes[a][...],
                    (((1,), (side,)), ((), ())),
                    preferred_element_type=f32,
                ),
            )

    def halo(buffer, length, i):
        return pltpu.make_async_remote_copy(
            src_ref=buffer.at[pl.ds(rows, length)],
            dst_ref=buffer.at[pl.ds(0, length)],
            send_sem=halo_send.at[i],
            recv_sem=halo_recv.at[i],
            device_id={"sp": right},
            device_id_type=MESH,
        )

    for a in range(QUERY):
        pass_on(a, 1, n)

    def store_kv(base, value):
        kv[pl.ds(base + WINDOW, tile), :] = value.astype(bf16)

    project(0, store_kv)

    @pl.when(jnp.logical_not(has_left))
    def _():
        kv[pl.ds(0, WINDOW), :] = jnp.zeros((WINDOW, kv.shape[1]), bf16)
        conv_in[pl.ds(0, PAD), :] = jnp.zeros((PAD, conv_in.shape[1]), f32)

    pass_on(QUERY, 1, n)

    @pl.when(has_right)
    def _():
        halo(kv, WINDOW, 0).start()

    def store_query(base, value):
        query[pl.ds(base, tile), :] = value.astype(bf16)

    project(QUERY, store_query)

    heads = query.shape[1] // HEAD_DIM
    query_idx = lax.broadcasted_iota(jnp.int32, (WINDOW, 2 * WINDOW), 0)
    key_idx = lax.broadcasted_iota(jnp.int32, (WINDOW, 2 * WINDOW), 1)
    gap = query_idx + WINDOW - key_idx
    band = (gap >= 0) & (gap < WINDOW)
    lane = lax.broadcasted_iota(jnp.int32, (2 * WINDOW, LANES), 1)
    low = lane < HEAD_DIM
    stat_lane = lax.broadcasted_iota(jnp.int32, (WINDOW, LANES), 1)

    def attend(b, kept):
        base = pl.multiple_of(b * WINDOW, WINDOW)
        both = kv[pl.ds(base, 2 * WINDOW), :].astype(f32)
        turned = pltpu.roll(both, HEAD_DIM, 1)
        zero = jnp.zeros_like(both)
        keys = (jnp.where(low, both, zero).astype(bf16), jnp.where(low, zero, turned).astype(bf16))
        vals = (jnp.where(low, turned, zero).astype(bf16), jnp.where(low, zero, both).astype(bf16))
        stats = jnp.zeros((WINDOW, LANES), f32)
        for pair in range(heads // 2):
            cols = pl.ds(pair * LANES, LANES)
            q = query[pl.ds(base, WINDOW), cols]
            out = None
            for side in range(2):
                head = 2 * pair + side
                scores = lax.dot_general(
                    q, keys[side], (((1,), (1,)), ((), ())), preferred_element_type=f32
                ) * HEAD_DIM ** (-0.5)
                scores = jnp.where(kept, scores, -jnp.inf)
                sink = jnp.full((WINDOW, 1), sink_ref[head], f32)
                top = jnp.maximum(jnp.max(scores, axis=-1, keepdims=True), sink)
                raised = jnp.exp(scores - top)
                total = jnp.sum(raised, axis=-1, keepdims=True) + jnp.exp(sink - top)
                weights = (raised * (1.0 / total)).astype(bf16)
                part = jnp.dot(weights, vals[side], preferred_element_type=f32)
                out = part if out is None else out + part
                stats = jnp.where(stat_lane == head, top + jnp.log(total), stats)
            attended[pl.ds(base, WINDOW), cols] = out
        log_ref[:, pl.ds(base, WINDOW)] = jnp.transpose(stats)[:heads]

    def attend_range(first, last):
        @pl.loop(first, last)
        def _(b):
            attend(b, band)

    cut = [1 + (n - 1) * i // 3 for i in range(4)]
    mid = 1 + (blocks - 1) // 2
    attend_range(1, mid)
    pass_on(CONV, cut[0], cut[1])
    attend_range(mid, blocks)
    pass_on(CONV, cut[1], cut[2])

    @pl.when(has_left)
    def _():
        halo(kv, WINDOW, 0).wait_recv()

    attend(0, band & ((key_idx >= WINDOW) | has_left))
    pass_on(CONV, cut[2], cut[3])

    def store_conv(base, value):
        conv_in[pl.ds(base + PAD, tile), :] = value.astype(bf16).astype(f32)

    project(CONV, store_conv)
    early = min(2, n - 1)
    pass_on(GATE, 1, early)

    @pl.when(has_right)
    def _():
        halo(conv_in, PAD, 1).start()

    pass_on(GATE, early, n - 1)

    far = jnp.where(2 * me >= n, 0, n - 1)

    def gate_part(base, shard):
        at = pl.ds(pl.multiple_of(shard * depth, depth), depth)
        return jnp.dot(
            normed[pl.ds(base, tile), at], cg_all[at, :], preferred_element_type=f32
        )

    if flip:

        @pl.loop(0, rows // tile)
        def _(i):
            base = pl.multiple_of(i * tile, tile)
            part = gate_part(base, lax.rem(far + 1, n))
            for j in range(2, n):
                part = part + gate_part(base, lax.rem(far + j, n))
            gate_sum[pl.ds(base, tile), :] = part

    pass_on(GATE, n - 1, n)

    @pl.when(has_left)
    def _():
        halo(conv_in, PAD, 1).wait_recv()

    def store_mixed(base, value):
        gate = value.astype(bf16).astype(f32)
        taps = taps_ref[...].astype(f32)
        near = conv_in[pl.ds(base, tile + PAD), :]
        total = jnp.zeros_like(gate)
        for k in range(TAPS):
            start = PAD - TAPS + 1 + k
            total = total + taps[k : k + 1] * near[start : start + tile]
        mixed_ref[pl.ds(base, tile), :] = (attended[pl.ds(base, tile), :] + gate * total).astype(bf16)

    if flip:

        @pl.loop(0, rows // tile)
        def _(i):
            base = pl.multiple_of(i * tile, tile)
            store_mixed(base, gate_sum[pl.ds(base, tile), :] + gate_part(base, far))

    else:
        project(GATE, store_mixed)

    @pl.when(has_right)
    def _():
        halo(kv, WINDOW, 0).wait_send()
        halo(conv_in, PAD, 1).wait_send()

    for a in range(arrays):

        @pl.when(has_right)
        def _():
            @pl.loop(0, me + 1)
            def _(s):
                hop(a, s, True).wait_send()

        @pl.when(has_left)
        def _():
            @pl.loop(me, n)
            def _(s):
                hop(a, s, False).wait_send()


def body(n, tokens, norm_gain, w_query, w_key, w_value, w_conv_in, w_conv_gate, conv_taps, sink_logits):
    rows, features = tokens.shape
    width, kv_width = w_query.shape[1], w_key.shape[1] + w_value.shape[1]
    assert w_key.shape[1] == HEAD_DIM and width % LANES == 0
    depth = w_query.shape[0]
    flip = depth % LANES == 0 and 2 < n <= 16
    if flip:
        w_kv, kv_shape = (w_key.T, w_value.T), (kv_width, features)
    else:
        w_kv, kv_shape = (jnp.concatenate([w_key, w_value], axis=1),), (features, kv_width)
    arrays = 3 + len(w_kv)
    f32, bf16 = jnp.float32, jnp.bfloat16
    hbm = pl.BlockSpec(memory_space=pltpu.HBM)
    vmem = pl.BlockSpec(memory_space=pltpu.VMEM)
    smem = pl.BlockSpec(memory_space=pltpu.SMEM)
    dma = pltpu.SemaphoreType.DMA
    return pl.pallas_call(
        functools.partial(kernel, n, flip),
        out_shape=(
            pltpu.VMEM((rows, width), bf16),
            pltpu.VMEM((width // HEAD_DIM, rows), f32),
        ),
        in_specs=[hbm, vmem] + [hbm] * arrays + [vmem, smem],
        out_specs=(vmem, vmem),
        scratch_shapes=[
            pltpu.VMEM((rows, features), bf16),
            pltpu.VMEM((rows, features), bf16),
            pltpu.VMEM(kv_shape, bf16),
            pltpu.VMEM((features, width), bf16),
            pltpu.VMEM((features, width), bf16),
            pltpu.VMEM((features, width), bf16),
            pltpu.VMEM((rows + WINDOW, kv_width), bf16),
            pltpu.VMEM((rows, width), bf16),
            pltpu.VMEM((rows, width), f32),
            pltpu.VMEM((rows + PAD, width), f32),
            pltpu.VMEM((rows, width), f32),
            dma((4,)),
            dma((arrays,)),
            dma((arrays, n)),
            dma((arrays, n)),
            dma((arrays, n)),
            dma((2,)),
            dma((2,)),
        ],
        compiler_params=pltpu.CompilerParams(
            collective_id=0, has_side_effects=True, vmem_limit_bytes=59 << 20
        ),
        name="gather_attend_convolve",
    )(tokens, norm_gain.reshape(1, -1), *w_kv, w_query, w_conv_in, w_conv_gate, conv_taps, sink_logits)


def solution(mesh):
    return jax.shard_map(
        functools.partial(body, mesh.shape["sp"]),
        mesh=mesh,
        in_specs=(
            P("sp", None),
            P(),
            P("sp", ("fs", "tp")),
            P("sp", ("fs", "tp")),
            P("sp", ("fs", "tp")),
            P("sp", ("fs", "tp")),
            P("sp", ("fs", "tp")),
            P(None, ("fs", "tp")),
            P(("fs", "tp")),
        ),
        out_specs=(P("sp", ("fs", "tp")), P(("fs", "tp"), "sp")),
        check_vma=False,
    )
```
